256 devices in a mesh: sp: 32 (over z, x), tp: 8 (over y, core).
Axes of the slice: x: 4, y: 4, z: 8, core: 2. Of those that a mesh axis runs over, the one named last changes fastest.
Arguments:
- latent: bfloat16 [73728, 2048], P(('sp', 'tp')), may hold values from -0.6 to 0.6
- context: bfloat16 [256, 2048], P(('sp', 'tp')), may hold values from -6 to 6
- condition: float32 [2048], P('sp'), may hold values from -6 to 6
- context_condition: float32 [2048], P('sp'), may hold values from -6 to 6
- modulation_weight: bfloat16 [2048, 6144], P('sp', 'tp'), may hold values from -0.1875 to 0.1875
- norm_gain: float32 [2048], replicated, may hold values from 0.1 to 1.9
- query_weight: bfloat16 [2048, 1024], replicated
- key_weight: bfloat16 [2048, 256], replicated
- value_weight: bfloat16 [2048, 256], replicated, may hold values from -0.125 to 0.125
- output_weight: bfloat16 [1024, 2048], replicated, may hold values from -0.1875 to 0.1875
- query_gain: float32 [128], replicated, may hold values from 0.5 to 6
- key_gain: float32 [128], replicated, may hold values from 0.5 to 6
- sink_logit: float32 [8], replicated, may hold values from 1 to 5
Outputs:
- updated: bfloat16 [73728, 2048], P(('sp', 'tp'))
The draws below stay inside these ranges and needn't reach their ends.
All inputs are finite; a program needn't handle non-finite values.
Results may differ from the reference program's by a relative error of at most 0.006.
The reference program's roundings to bfloat16 on the way count: a program that leaves them out, or rounds other values in their place, can miss the bound.
Values may be sent and summed in bfloat16 or wider, within the bound.
No kernel may reach another device: no remote copies, remote signals or barrier semaphores. Data moves between devices by JAX's collectives and lax.ppermute only.
A program may use at most 64 MiB of HBM per device.

```python
import jax
import jax.numpy as jnp
from jax import lax

D = 2048
HEADS = 8
KV_HEADS = 2
HEAD = 128
WINDOW = 128
GRID_W = 64
TOK_DEV = 288
TOKENS = 73728
CONTEXT = 256


def draw_latent(key, part):
    normal_rows = jnp.clip(jax.random.normal(jax.random.fold_in(key, 1), (TOKENS, D), jnp.float32), -6.0, 6.0)
    return (0.1 * normal_rows).astype(jnp.bfloat16)


def shared_keys(key):
    drawn = jax.random.normal(jax.random.fold_in(key, 21), (D, KV_HEADS * HEAD), jnp.float32)
    return jnp.clip(drawn, -4.0, 4.0) * D ** (-0.5)


def draw_key_weight(key, part):
    return shared_keys(key).astype(jnp.bfloat16)


def draw_query_weight(key, part):
    drawn = jax.random.normal(jax.random.fold_in(key, 22), (D, HEADS * HEAD), jnp.float32)
    drawn = jnp.clip(drawn, -4.0, 4.0) * D ** (-0.5)
    return drawn.astype(jnp.bfloat16)


def draw_query_gain(key, part):
    return jax.random.uniform(jax.random.fold_in(key, 32), (HEAD,), jnp.float32, 0.5, 1.6)


def draw_key_gain(key, part):
    return jax.random.uniform(jax.random.fold_in(key, 34), (HEAD,), jnp.float32, 0.5, 1.6)


def steps_of(rng, shape, pieces, smallest, largest):
    factor_of, own = 1.0, jax.random.fold_in(rng, 6)
    for axis_at, blocks in pieces:
        heights = jnp.exp(jax.random.uniform(jax.random.fold_in(own, axis_at), (blocks,), jnp.float32, smallest / len(pieces), largest / len(pieces)))
        factor_of = factor_of * jnp.repeat(heights, shape[axis_at] // blocks).reshape([-1 if axis == axis_at else 1 for axis in range(len(shape))])
    return factor_of


def bell_draw(key, shape, deviation, bound, cuts=(), kind=jnp.bfloat16):
    entries = jax.random.normal(key, shape, jnp.float32) * deviation
    if len(cuts) > 0:
        entries = steps_of(key, shape, cuts, -0.22, 0.18) * entries
    return jnp.clip(entries, min=-bound, max=bound).astype(kind)


def setup_inputs(seed: int = 0) -> dict:
    key_of = jax.random.split(jax.random.key(seed), 14)
    latent = draw_latent(jax.random.fold_in(key_of[13], 71), 0)
    context = bell_draw(key_of[1], (CONTEXT, D), 1.0, 6.0, ((0, 256),))
    condition = bell_draw(key_of[2], (D,), 1.0, 6.0, ((0, 32),), jnp.float32)
    context_condition = bell_draw(key_of[3], (D,), 1.0, 6.0, ((0, 32),), jnp.float32)
    modulation_weight = bell_draw(key_of[4], (D, 3 * D), (D // 2) ** -0.5, 0.1875, ((0, 32), (1, 8)))
    norm_gain = jnp.clip(1.0 + 0.18 * jax.random.normal(key_of[5], (D,), jnp.float32), 0.1, 1.9)
    query_weight = draw_query_weight(jax.random.fold_in(key_of[13], 71), 0)
    key_weight = draw_key_weight(jax.random.fold_in(key_of[13], 71), 0)
    value_weight = bell_draw(key_of[8], (D, KV_HEADS * HEAD), D ** -0.5, 0.125)
    output_weight = bell_draw(key_of[9], (HEADS * HEAD, D), (HEADS * HEAD) ** -0.5, 0.1875)
    query_gain = draw_query_gain(jax.random.fold_in(key_of[13], 71), 0)
    key_gain = draw_key_gain(jax.random.fold_in(key_of[13], 71), 0)
    sink_logit = jnp.clip(jax.random.uniform(key_of[12], (HEADS,), jnp.float32, 1.0, 5.0), 1.0, 5.0)
    return dict(latent=latent, context=context, condition=condition, context_condition=context_condition, modulation_weight=modulation_weight, norm_gain=norm_gain, query_weight=query_weight, key_weight=key_weight, value_weight=value_weight, output_weight=output_weight, query_gain=query_gain, key_gain=key_gain, sink_logit=sink_logit)


EPS = 1e-06
ROPE_BASE = 10000.0
FAR_LOGIT = -1e+30

def rms_rows(values_in):
    return values_in * lax.rsqrt(lax.optimization_barrier(jnp.mean(values_in * values_in, axis=-1, keepdims=True)) + EPS)

def turn_halves(halves_in):
    former, latter = jnp.split(halves_in, 2, axis=-1)
    return jnp.concatenate([-latter, former], axis=-1)

def rotary(values_in, positions):
    quarter = values_in.shape[-1] // 4
    inverse = jnp.power(ROPE_BASE, -jnp.arange(quarter, dtype=jnp.float32) / quarter)
    by_rows = (positions // GRID_W).astype(jnp.float32)[:, None] * inverse
    by_cols = (positions % GRID_W).astype(jnp.float32)[:, None] * inverse
    angles = jnp.concatenate([by_rows, by_rows, by_cols, by_cols], axis=-1)[:, None, :]
    row_half, col_half = jnp.split(values_in, 2, axis=-1)
    turned = jnp.concatenate([turn_halves(row_half), turn_halves(col_half)], axis=-1)
    return values_in * jnp.cos(angles) + turned * jnp.sin(angles)

def head_norm(flat, gain):
    per_head = flat.reshape(flat.shape[0], flat.shape[1] // gain.shape[0], gain.shape[0])
    return rms_rows(per_head) * gain

def modulated(tokens_in, norm_gain, shift, scale):
    values_in = tokens_in.astype(jnp.float32)
    return (rms_rows(values_in) * norm_gain * (1.0 + scale) + shift).astype(jnp.bfloat16)

def project_ctx(ctx_hidden, key_weight, value_weight, key_gain):
    row_count = ctx_hidden.shape[0]
    ctx_keys = head_norm(jnp.dot(ctx_hidden, key_weight, preferred_element_type=jnp.float32), key_gain)
    ctx_keys = ctx_keys.astype(jnp.bfloat16).reshape(row_count, -1)
    ctx_values = jnp.dot(ctx_hidden, value_weight, preferred_element_type=jnp.float32).astype(jnp.bfloat16)
    return (ctx_keys, ctx_values)

def attend(queries, keys, values, ctx_keys, ctx_values, sink_logit, allowed, head_size):
    row_count = queries.shape[0]
    kv_count = keys.shape[1] // head_size
    group = queries.shape[1] // keys.shape[1]
    score_scale = head_size ** (-0.5)
    grouped = queries.astype(jnp.float32).reshape(row_count, kv_count, group, head_size)
    near_keys = keys.astype(jnp.float32).reshape(-1, kv_count, head_size)
    near_values = values.astype(jnp.float32).reshape(-1, kv_count, head_size)
    far_keys = ctx_keys.astype(jnp.float32).reshape(-1, kv_count, head_size)
    far_values = ctx_values.astype(jnp.float32).reshape(-1, kv_count, head_size)
    near_scores = jnp.einsum('rhgd,khd->hgrk', grouped, near_keys) * score_scale
    near_scores = jnp.where(allowed, near_scores, FAR_LOGIT)
    ctx_scores = jnp.einsum('rhgd,khd->hgrk', grouped, far_keys) * score_scale
    sink_part = sink_logit.reshape(kv_count, group)[:, :, None, None]
    row_max = jnp.maximum(jnp.maximum(lax.optimization_barrier(jnp.max(near_scores, axis=-1, keepdims=True)), lax.optimization_barrier(jnp.max(ctx_scores, axis=-1, keepdims=True))), sink_part)
    near_exp = jnp.exp(near_scores - row_max)
    ctx_exp = jnp.exp(ctx_scores - row_max)
    denominator = lax.optimization_barrier(jnp.sum(near_exp, axis=-1, keepdims=True)) + lax.optimization_barrier(jnp.sum(ctx_exp, axis=-1, keepdims=True)) + jnp.exp(sink_part - row_max)
    near_probs = (near_exp / denominator).astype(jnp.bfloat16).astype(jnp.float32)
    ctx_probs = (ctx_exp / denominator).astype(jnp.bfloat16).astype(jnp.float32)
    mixed = jnp.einsum('hgrk,khd->rhgd', near_probs, near_values) + jnp.einsum('hgrk,khd->rhgd', ctx_probs, far_values)
    return mixed.astype(jnp.bfloat16).reshape(row_count, -1)

def reference(latent, context, condition, context_condition, modulation_weight, norm_gain, query_weight, key_weight, value_weight, output_weight, query_gain, key_gain, sink_logit):
    model_width = latent.shape[1]
    head_size = query_gain.shape[0]
    activations = jax.nn.silu(jnp.stack([condition, context_condition])).astype(jnp.bfloat16)
    modulation = jnp.dot(activations, modulation_weight, preferred_element_type=jnp.float32)
    hidden = modulated(latent, norm_gain, modulation[0, :model_width], modulation[0, model_width:2 * model_width])
    ctx_hidden = modulated(context, norm_gain, modulation[1, :model_width], modulation[1, model_width:2 * model_width])
    gate = modulation[0, 2 * model_width:]
    positions = jnp.arange(TOKENS, dtype=jnp.int32)
    queries = rotary(head_norm(jnp.dot(hidden, query_weight, preferred_element_type=jnp.float32), query_gain), positions).astype(jnp.bfloat16).reshape(TOKENS, -1)
    keys = rotary(head_norm(jnp.dot(hidden, key_weight, preferred_element_type=jnp.float32), key_gain), positions).astype(jnp.bfloat16).reshape(TOKENS, -1)
    values = jnp.dot(hidden, value_weight, preferred_element_type=jnp.float32).astype(jnp.bfloat16)
    ctx_keys, ctx_values = project_ctx(ctx_hidden, key_weight, value_weight, key_gain)
    padded_keys = jnp.pad(keys, ((WINDOW, WINDOW), (0, 0)))
    padded_values = jnp.pad(values, ((WINDOW, WINDOW), (0, 0)))

    def one_block(block_index):
        first_row = block_index * TOK_DEV
        query_block = lax.dynamic_slice_in_dim(queries, first_row, TOK_DEV, 0)
        key_block = lax.dynamic_slice_in_dim(padded_keys, first_row, TOK_DEV + 2 * WINDOW, 0)
        value_block = lax.dynamic_slice_in_dim(padded_values, first_row, TOK_DEV + 2 * WINDOW, 0)
        latent_block = lax.dynamic_slice_in_dim(latent, first_row, TOK_DEV, 0)
        query_pos = first_row + jnp.arange(TOK_DEV, dtype=jnp.int32)
        key_pos = first_row - WINDOW + jnp.arange(TOK_DEV + 2 * WINDOW, dtype=jnp.int32)
        allowed = (jnp.abs(key_pos[None, :] - query_pos[:, None]) <= WINDOW) & (key_pos[None, :] >= 0) & (key_pos[None, :] < TOKENS)
        mixed = attend(query_block, key_block, value_block, ctx_keys, ctx_values, sink_logit, allowed, head_size)
        update = jnp.dot(mixed, output_weight, preferred_element_type=jnp.float32)
        return (latent_block.astype(jnp.float32) + gate * update).astype(jnp.bfloat16)
    blocks = lax.map(one_block, jnp.arange(TOKENS // TOK_DEV, dtype=jnp.int32))
    return blocks.reshape(TOKENS, model_width)
```

```python
import functools

import jax
import jax.numpy as jnp
from jax import lax
from jax.experimental import pallas as pl
from jax.experimental.pallas import tpu as pltpu
from jax.sharding import Mesh
from jax.sharding import PartitionSpec as P

WINDOW = 128
GRID_W = 64
HEAD = 128
HEADS = 8
KV_HEADS = 2
GROUP = HEADS // KV_HEADS
CHUNK = 96
EPS = 1e-06
ROPE_BASE = 10000.0
FAR_LOGIT = -1e30
LOG2E = 1.4426950408889634
MIB = 1024 * 1024
ALL_VMEM = 67_043_328
GROUP_ROWS = 32

AXES = ("z", "x", "y", "c")
FIRST = ("z", "c")
SECOND = ("x", "y")

F32 = jnp.float32
BF16 = jnp.bfloat16


def rms_scale(v):
    return lax.rsqrt(jnp.mean(v * v, axis=-1, keepdims=True) + EPS)


def high_low(v):
    high = v.astype(BF16).astype(F32)
    return high, v - high


def exchange(array, axes):
    return lax.all_to_all(array, axes, split_axis=0, concat_axis=0, tiled=True)


def copy_all(pairs, sems):
    copies = [
        pltpu.make_async_copy(src, dst, sems.at[i]) for i, (src, dst) in enumerate(pairs)
    ]
    for copy in copies:
        copy.start()
    return copies


def partial_kernel(
    cond_hbm, cctx_hbm, weight_hbm, ctx_hbm, out_ref,
    cond_ref, cctx_ref, weight_ref, ctx_ref, act_ref, rows_ref, sems,
):
    copies = copy_all(
        [(cond_hbm, cond_ref), (cctx_hbm, cctx_ref), (weight_hbm, weight_ref), (ctx_hbm, ctx_ref)],
        sems,
    )
    width = weight_ref.shape[1]
    model = ctx_ref.shape[1]
    act_ref[...] = jnp.zeros_like(act_ref)
    rows_ref[...] = jnp.zeros_like(rows_ref)
    for copy in copies:
        copy.wait()
    act_ref[0:1, :] = jax.nn.silu(cond_ref[...])
    act_ref[1:2, :] = jax.nn.silu(cctx_ref[...])
    part = jnp.dot(act_ref[...].astype(BF16), weight_ref[...], preferred_element_type=F32)
    high, low = high_low(part)
    rows_ref[0:2, :] = high[0:2]
    rows_ref[2:4, :] = low[0:2]
    ctx = ctx_ref[...].astype(F32)
    for i in range(3):
        size = min(width, model - i * width)
        rows_ref[4 + i : 5 + i, 0:size] = ctx[:, i * width : i * width + size]
    packed = rows_ref[...].astype(BF16)
    for i in range(out_ref.shape[0]):
        out_ref[i] = packed


def edges_kernel(lat_hbm, low_ref, high_ref, sems):
    own = lat_hbm.shape[0]
    copies = copy_all(
        [
            (lat_hbm.at[pl.ds(0, WINDOW)], low_ref),
            (lat_hbm.at[pl.ds(own - WINDOW, WINDOW)], high_ref),
        ],
        sems,
    )
    for copy in copies:
        copy.wait()


def middle_kernel(in_ref, out_ref, ctx_out, rows_ref, ctx_ref):
    members, _, width = in_ref.shape
    model = ctx_out.shape[1]
    for c in range(2):
        total = None
        for z in range(members // 2):
            m = 2 * z + c
            rows = in_ref[m].astype(F32)
            total = rows if total is None else total + rows
            for i in range(3):
                size = min(width, model - i * width)
                ctx_ref[m : m + 1, i * width : i * width + size] = rows[4 + i : 5 + i, 0:size]
        rows_ref[0:8, :] = total
        high, low = high_low(rows_ref[0:2, :] + rows_ref[2:4, :])
        rows_ref[8 + 4 * c : 10 + 4 * c, :] = high
        rows_ref[10 + 4 * c : 12 + 4 * c, :] = low
    packed = rows_ref[8:16, :].astype(BF16)
    for i in range(out_ref.shape[0]):
        out_ref[i] = packed
    ctx_out[...] = ctx_ref[...].astype(BF16)


def context_kernel(
    second_ref, c0_ref, c1_ref, c2_ref, c3_ref, gain_ref, wk_ref, wv_ref, kgain_ref,
    kv_out, vec_out, mod_ref, tmp_ref, hid_ref,
):
    members, _, width = second_ref.shape
    model = gain_ref.shape[1]
    side = 4
    for y in range(side):
        total = second_ref[y].astype(F32)
        for x in range(1, members // side):
            total += second_ref[x * side + y].astype(F32)
        tmp_ref[...] = total
        for c in range(2):
            at = (2 * y + c) * width
            mod_ref[0:2, at : at + width] = (
                tmp_ref[4 * c : 4 * c + 2, :] + tmp_ref[4 * c + 2 : 4 * c + 4, :]
            )
    gain = gain_ref[...]
    vec_out[0:1, :] = gain * (1.0 + mod_ref[0:1, model : 2 * model])
    vec_out[1:2, :] = mod_ref[0:1, 0:model]
    vec_out[2:3, :] = mod_ref[0:1, 2 * model : 3 * model]
    scale = gain * (1.0 + mod_ref[1:2, model : 2 * model])
    shift = mod_ref[1:2, 0:model]
    for i, ref in enumerate((c0_ref, c1_ref, c2_ref, c3_ref)):
        rows = ref[...].astype(F32)
        n = rows.shape[0]
        hid_ref[i * n : (i + 1) * n, :] = (rows * rms_scale(rows) * scale + shift).astype(BF16)
    keys = jnp.dot(hid_ref[...], wk_ref[...], preferred_element_type=F32)
    kv_out[:, KV_HEADS * HEAD :] = jnp.dot(
        hid_ref[...], wv_ref[...], preferred_element_type=F32
    ).astype(BF16)
    for h in range(KV_HEADS):
        k = keys[:, h * HEAD : (h + 1) * HEAD]
        kv_out[:, h * HEAD : (h + 1) * HEAD] = (k * rms_scale(k) * kgain_ref[...]).astype(BF16)


def turn(v, table_ref, first, group, groups):
    turned = jnp.where(first, pltpu.roll(v, HEAD - 32, 1), pltpu.roll(v, 32, 1))
    parts = []
    for i in range(groups):
        rows = slice(i * GROUP_ROWS, (i + 1) * GROUP_ROWS)
        at = pl.ds((group + i) * GROUP_ROWS, GROUP_ROWS)
        parts.append((v[rows] * table_ref[0, at, :] + turned[rows] * table_ref[1, at, :]).astype(BF16))
    return jnp.concatenate(parts, axis=0)


def project_kernel(
    start_ref, low_ref, mid_ref, high_ref, vec_ref, wk_ref, wv_ref, qgain_ref, kgain_ref,
    row_ref, col_ref, wq_hbm,
    q_out, k_out, v_out, hid_ref, table_ref, wq_ref, sem,
):
    load = pltpu.make_async_copy(wq_hbm, wq_ref, sem)
    load.start()
    own = mid_ref.shape[0]
    rows = own + 2 * WINDOW
    scale = vec_ref[0:1, :]
    shift = vec_ref[1:2, :]
    at = 0
    for ref in (low_ref, mid_ref, high_ref):
        for r in range(0, ref.shape[0], 32):
            v = ref[r : r + 32, :].astype(F32)
            hid_ref[at : at + 32, :] = (v * rms_scale(v) * scale + shift).astype(BF16)
            at += 32
    block = start_ref[0] // GROUP_ROWS - WINDOW // GROUP_ROWS
    first_row = lax.shift_right_arithmetic(block, 1)
    for i in range(rows // GROUP_ROWS):
        row = lax.shift_right_arithmetic(block + i, 1) - first_row
        half = lax.bitwise_and(block + i, 1) * GROUP_ROWS
        for t in range(2):
            table_ref[t, i * GROUP_ROWS : (i + 1) * GROUP_ROWS, :] = (
                row_ref[t, pl.ds(row, 1), :] + col_ref[t, pl.ds(half, GROUP_ROWS), :]
            )
    lane = lax.broadcasted_iota(jnp.int32, (1, HEAD), 1)
    first = (lane % 64) < 32
    v_out[...] = jnp.dot(hid_ref[...], wv_ref[...], preferred_element_type=F32).astype(BF16)
    keys = jnp.dot(hid_ref[...], wk_ref[...], preferred_element_type=F32)
    kgain = kgain_ref[...]
    for h in range(KV_HEADS):
        k = keys[:, h * HEAD : (h + 1) * HEAD]
        k = k * rms_scale(k) * kgain
        k_out[:, h * HEAD : (h + 1) * HEAD] = turn(k, table_ref, first, 0, rows // GROUP_ROWS)
    qgain = qgain_ref[...]
    load.wait()
    for pair in range(HEADS // 2):
        at = pair * 2 * HEAD
        both = jnp.dot(
            hid_ref[WINDOW : WINDOW + own, :], wq_ref[:, at : at + 2 * HEAD],
            preferred_element_type=F32,
        )
        for h in range(2):
            q = both[:, h * HEAD : (h + 1) * HEAD]
            q = q * rms_scale(q) * qgain
            q = turn(q, table_ref, first, WINDOW // GROUP_ROWS, own // GROUP_ROWS)
            for c in range(own // CHUNK):
                q_out[c, 2 * pair + h] = q[c * CHUNK : (c + 1) * CHUNK]


def attend_kernel(
    start_ref, sink_ref, q_ref, k_ref, v_ref, x0_ref, x1_ref, x2_ref, x3_ref, lat_ref, vec_ref,
    wo_hbm, out_ref, mix_ref, vals_ref, ctx_ref, wo_ref, sem, *, total_rows,
):
    load = pltpu.make_async_copy(wo_hbm, wo_ref, sem)
    load.start()
    chunks = q_ref.shape[0]
    rows = k_ref.shape[0]
    far = ctx_ref.shape[0]
    for i, ref in enumerate((x0_ref, x1_ref, x2_ref, x3_ref)):
        n = ref.shape[0]
        ctx_ref[i * n : (i + 1) * n, :] = ref[...]
    width = CHUNK + 2 * WINDOW
    factor = HEAD ** (-0.5) * LOG2E
    kv = KV_HEADS * HEAD
    for g in range(KV_HEADS):
        vals_ref[g, 0:rows, 0:HEAD] = v_ref[:, g * HEAD : (g + 1) * HEAD]
        vals_ref[g, rows : rows + far, 0:HEAD] = ctx_ref[:, kv + g * HEAD : kv + (g + 1) * HEAD]
        vals_ref[g, :, HEAD:] = jnp.ones_like(vals_ref[g, :, HEAD:])
    row = lax.broadcasted_iota(jnp.int32, (CHUNK, width), 0)
    col = lax.broadcasted_iota(jnp.int32, (CHUNK, width), 1)
    nt = (((1,), (1,)), ((), ()))
    for c in range(chunks):
        pos = start_ref[0] - WINDOW + c * CHUNK + col
        allowed = (col >= row) & (col <= row + 2 * WINDOW) & (pos >= 0) & (pos < total_rows)
        bias = jnp.where(allowed, 0.0, FAR_LOGIT)
        for g in range(KV_HEADS):
            q = q_ref[c, g * GROUP : (g + 1) * GROUP].reshape(GROUP * CHUNK, HEAD)
            k = k_ref[c * CHUNK : c * CHUNK + width, g * HEAD : (g + 1) * HEAD]
            near = lax.dot_general(q, k, nt, preferred_element_type=F32)
            near = near.reshape(GROUP, CHUNK, width) + bias[None]
            ctx = lax.dot_general(
                q, ctx_ref[:, g * HEAD : (g + 1) * HEAD], nt, preferred_element_type=F32
            ).reshape(GROUP, CHUNK, far)
            sink = jnp.concatenate(
                [jnp.full((1, CHUNK, 1), sink_ref[g * GROUP + h], F32) for h in range(GROUP)], axis=0
            ) * (HEAD**0.5)
            top = jnp.maximum(
                jnp.maximum(
                    jnp.max(near, axis=-1, keepdims=True), jnp.max(ctx, axis=-1, keepdims=True)
                ),
                sink,
            )
            near = jnp.exp2((near - top) * factor).astype(BF16).reshape(GROUP * CHUNK, width)
            ctx = jnp.exp2((ctx - top) * factor).astype(BF16).reshape(GROUP * CHUNK, far)
            tail = jnp.exp2((sink - top) * factor).reshape(GROUP * CHUNK, 1)
            mixed = jnp.dot(
                near, vals_ref[g, c * CHUNK : c * CHUNK + width, :], preferred_element_type=F32
            ) + jnp.dot(ctx, vals_ref[g, rows : rows + far, :], preferred_element_type=F32)
            mixed = (mixed[:, :HEAD] / (mixed[:, HEAD:] + tail)).astype(BF16)
            for h in range(GROUP):
                at = (g * GROUP + h) * HEAD
                mix_ref[c * CHUNK : (c + 1) * CHUNK, at : at + HEAD] = mixed[
                    h * CHUNK : (h + 1) * CHUNK
                ]
    model = out_ref.shape[1]
    load.wait()
    for at in range(0, model, 256):
        update = jnp.dot(mix_ref[...], wo_ref[:, at : at + 256], preferred_element_type=F32)
        out_ref[:, at : at + 256] = (
            lat_ref[:, at : at + 256].astype(F32) + vec_ref[2:3, at : at + 256] * update
        ).astype(BF16)


def call(kernel, outs, scratch, limit, flops, *args, smem=0, hbm=()):
    vmem = pl.BlockSpec(memory_space=pltpu.VMEM)
    many = isinstance(outs, (list, tuple))
    specs = [pl.BlockSpec(memory_space=pltpu.SMEM)] * smem + [vmem] * (len(args) - smem)
    for i in hbm:
        specs[i] = pl.BlockSpec(memory_space=pltpu.HBM)
    return pl.pallas_call(
        kernel,
        out_shape=outs,
        in_specs=specs,
        out_specs=[vmem] * len(outs) if many else vmem,
        scratch_shapes=scratch,
        compiler_params=pltpu.CompilerParams(vmem_limit_bytes=limit),
        cost_estimate=pl.CostEstimate(flops=flops, bytes_accessed=flops // 256, transcendentals=0),
    )(*args)


def rotary_tables(first_row, rows):
    quarter = HEAD // 4
    inverse = jnp.power(ROPE_BASE, -jnp.arange(quarter, dtype=F32) / quarter)
    sign = jnp.where(jnp.arange(HEAD // 2) < HEAD // 4, -1.0, 1.0)

    def table(positions):
        angles = positions.astype(F32)[:, None] * inverse
        angles = jnp.concatenate([angles, angles], axis=-1)
        return jnp.stack([jnp.cos(angles), jnp.sin(angles) * sign])

    by_rows = table(first_row + jnp.arange(rows, dtype=jnp.int32))
    by_cols = table(jnp.arange(GRID_W, dtype=jnp.int32))
    none = ((0, 0), (0, 0))
    return (
        jnp.pad(by_rows, (*none, (0, HEAD // 2))),
        jnp.pad(by_cols, (*none, (HEAD // 2, 0))),
    )


def spread(array, axis):
    size = lax.axis_size(axis)
    return [array] + [
        lax.ppermute(array, axis, [(i, (i + k) % size) for i in range(size)])
        for k in range(1, size)
    ]


def local(
    latent,
    context,
    condition,
    context_condition,
    modulation_weight,
    norm_gain,
    query_weight,
    key_weight,
    value_weight,
    output_weight,
    query_gain,
    key_gain,
    sink_logit,
):
    own, model = latent.shape
    width = modulation_weight.shape[1]
    kv = key_weight.shape[1]
    world = lax.axis_size(AXES)
    members = lax.axis_size(FIRST)
    start = lax.axis_index(AXES) * own
    total_rows = own * world
    up = [(i, i + 1) for i in range(world - 1)]
    down = [(i + 1, i) for i in range(world - 1)]
    struct = jax.ShapeDtypeStruct
    span = own + 2 * WINDOW
    start_ref = start.astype(jnp.int32)[None]

    payload = call(
        partial_kernel,
        struct((members, 8, width), BF16),
        [
            pltpu.VMEM((1, condition.shape[0]), F32),
            pltpu.VMEM((1, condition.shape[0]), F32),
            pltpu.VMEM(modulation_weight.shape, BF16),
            pltpu.VMEM((1, model), BF16),
            pltpu.VMEM((8, condition.shape[0]), F32),
            pltpu.VMEM((8, width), F32),
            pltpu.SemaphoreType.DMA((4,)),
        ],
        ALL_VMEM, 1000,
        condition[None], context_condition[None], modulation_weight, context,
        hbm=(0, 1, 2, 3),
    )
    with jax.named_scope("first"):
        first = exchange(payload, FIRST)
    with jax.named_scope("edges"):
        low, high = call(
            edges_kernel,
            [struct((WINDOW, model), BF16), struct((WINDOW, model), BF16)],
            [pltpu.SemaphoreType.DMA((2,))],
            ALL_VMEM, 1000,
            latent,
            hbm=(0,),
        )
    with jax.named_scope("halo"):
        below = lax.ppermute(high, AXES, up)
        above = lax.ppermute(low, AXES, down)
    by_rows, by_cols = rotary_tables(lax.div(start - WINDOW, GRID_W), 16)

    payload, ctx_rows = call(
        middle_kernel,
        [struct((lax.axis_size(SECOND), 8, width), BF16), struct((members, model), BF16)],
        [pltpu.VMEM((16, width), F32), pltpu.VMEM((members, model), F32)],
        4 * MIB, 1000,
        first,
    )
    with jax.named_scope("second"):
        second = exchange(payload, SECOND)
    with jax.named_scope("rows"):
        ctx_parts = spread(ctx_rows, "x")
    ctx_kv, vectors = call(
        context_kernel,
        [struct((4 * members, 2 * kv), BF16), struct((8, model), F32)],
        [
            pltpu.VMEM((8, 3 * model), F32),
            pltpu.VMEM((8, width), F32),
            pltpu.VMEM((4 * members, model), BF16),
        ],
        8 * MIB, 4_000_000_000,
        second, *ctx_parts, norm_gain[None], key_weight, value_weight, key_gain[None],
    )
    with jax.named_scope("pairs"):
        ctx_all = spread(ctx_kv, "y")
    queries, keys, values = call(
        project_kernel,
        [
            struct((own // CHUNK, HEADS, CHUNK, HEAD), BF16),
            struct((span, kv), BF16),
            struct((span, kv), BF16),
        ],
        [
            pltpu.VMEM((span, model), BF16),
            pltpu.VMEM((2, span, HEAD), F32),
            pltpu.VMEM(query_weight.shape, BF16),
            pltpu.SemaphoreType.DMA,
        ],
        20 * MIB, 6_000_000_000,
        start_ref, below, latent, above, vectors, key_weight, value_weight,
        query_gain[None], key_gain[None], by_rows, by_cols, query_weight,
        smem=1, hbm=(11,),
    )
    return call(
        functools.partial(attend_kernel, total_rows=total_rows),
        struct((own, model), BF16),
        [
            pltpu.VMEM((own, HEADS * HEAD), BF16),
            pltpu.VMEM((KV_HEADS, span + world, 2 * HEAD), BF16),
            pltpu.VMEM((world, 2 * kv), BF16),
            pltpu.VMEM(output_weight.shape, BF16),
            pltpu.SemaphoreType.DMA,
        ],
        20 * MIB, 3_000_000_000,
        start_ref, sink_logit, queries, keys, values, *ctx_all, latent, vectors, output_weight,
        smem=2, hbm=(11,),
    )


def solution(mesh):
    torus = Mesh(mesh.devices.reshape(8, 4, 4, 2), AXES)
    rows = P(AXES, None)
    in_specs = (
        rows,
        rows,
        P(("z", "x")),
        P(("z", "x")),
        P(("z", "x"), ("y", "c")),
        P(),
        P(),
        P(),
        P(),
        P(),
        P(),
        P(),
        P(),
    )
    return jax.shard_map(local, mesh=torus, in_specs=in_specs, out_specs=rows, check_vma=False)
```

```python
import jax
import jax.numpy as jnp
from jax import lax
from jax.experimental import pallas as pl
from jax.experimental.pallas import tpu as pltpu
from jax.sharding import Mesh
from jax.sharding import PartitionSpec as P

WINDOW = 128
GRID_W = 64
HEAD = 128
HEADS = 8
KV_HEADS = 2
GROUP = HEADS // KV_HEADS
CHUNK = 96
EPS = 1e-06
ROPE_BASE = 10000.0
FAR_LOGIT = -1e30
LOG2E = 1.4426950408889634
MIB = 1024 * 1024
ALL_VMEM = 67_043_328
GROUP_ROWS = 32

AXES = ("z", "x", "y", "c")
FIRST = ("z", "c")
SECOND = ("x", "y")

F32 = jnp.float32
BF16 = jnp.bfloat16


def rms_scale(v):
    return lax.rsqrt(jnp.mean(v * v, axis=-1, keepdims=True) + EPS)


def high_low(v):
    high = v.astype(BF16).astype(F32)
    return high, v - high


def exchange(array, axes):
    return lax.all_to_all(array, axes, split_axis=0, concat_axis=0, tiled=True)


def copy_all(pairs, sems):
    copies = [
        pltpu.make_async_copy(src, dst, sems.at[i]) for i, (src, dst) in enumerate(pairs)
    ]
    for copy in copies:
        copy.start()
    return copies


def partial_kernel(
    cond_hbm, cctx_hbm, weight_hbm, ctx_hbm, out_ref,
    cond_ref, cctx_ref, weight_ref, ctx_ref, act_ref, rows_ref, sems,
):
    copies = copy_all(
        [(cond_hbm, cond_ref), (cctx_hbm, cctx_ref), (weight_hbm, weight_ref), (ctx_hbm, ctx_ref)],
        sems,
    )
    width = weight_ref.shape[1]
    model = ctx_ref.shape[1]
    act_ref[...] = jnp.zeros_like(act_ref)
    rows_ref[...] = jnp.zeros_like(rows_ref)
    for copy in copies:
        copy.wait()
    act_ref[0:1, :] = jax.nn.silu(cond_ref[...])
    act_ref[1:2, :] = jax.nn.silu(cctx_ref[...])
    part = jnp.dot(act_ref[...].astype(BF16), weight_ref[...], preferred_element_type=F32)
    high, low = high_low(part)
    rows_ref[0:2, :] = high[0:2]
    rows_ref[2:4, :] = low[0:2]
    ctx = ctx_ref[...].astype(F32)
    for i in range(3):
        size = min(width, model - i * width)
        rows_ref[4 + i : 5 + i, 0:size] = ctx[:, i * width : i * width + size]
    packed = rows_ref[...].astype(BF16)
    for i in range(out_ref.shape[0]):
        out_ref[i] = packed


def edges_kernel(lat_hbm, low_ref, high_ref, sems):
    own = lat_hbm.shape[0]
    copies = copy_all(
        [
            (lat_hbm.at[pl.ds(0, WINDOW)], low_ref),
            (lat_hbm.at[pl.ds(own - WINDOW, WINDOW)], high_ref),
        ],
        sems,
    )
    for copy in copies:
        copy.wait()


def middle_kernel(in_ref, out_ref, ctx_out, rows_ref, ctx_ref):
    members, _, width = in_ref.shape
    model = ctx_out.shape[1]
    for c in range(2):
        total = None
        for z in range(members // 2):
            m = 2 * z + c
            rows = in_ref[m].astype(F32)
            total = rows if total is None else total + rows
            for i in range(3):
                size = min(width, model - i * width)
                ctx_ref[m : m + 1, i * width : i * width + size] = rows[4 + i : 5 + i, 0:size]
        rows_ref[0:8, :] = total
        high, low = high_low(rows_ref[0:2, :] + rows_ref[2:4, :])
        rows_ref[8 + 4 * c : 10 + 4 * c, :] = high
        rows_ref[10 + 4 * c : 12 + 4 * c, :] = low
    packed = rows_ref[8:16, :].astype(BF16)
    for i in range(out_ref.shape[0]):
        out_ref[i] = packed
    ctx_out[...] = ctx_ref[...].astype(BF16)


def vectors_kernel(
    second_ref, mod_out, tmp_ref
):
    members, _, width = second_ref.shape
    side = 4
    for y in range(side):
        total = second_ref[y].astype(F32)
        for x in range(1, members // side):
            total += second_ref[x * side + y].astype(F32)
        tmp_ref[...] = total
        for c in range(2):
            at = (2 * y + c) * width
            mod_out[0:2, at : at + width] = (
                tmp_ref[4 * c : 4 * c + 2, :] + tmp_ref[4 * c + 2 : 4 * c + 4, :]
            )


def join_kernel(c0_ref, c1_ref, c2_ref, c3_ref, out_ref):
    for i, ref in enumerate((c0_ref, c1_ref, c2_ref, c3_ref)):
        n = ref.shape[0]
        out_ref[i * n : (i + 1) * n, :] = ref[...]


def context_kernel(
    mod_ref, ctx_ref, gain_ref, wk_ref, wv_ref, kgain_ref, kv_out, vec_out, hid_ref
):
    model = gain_ref.shape[1]
    gain = gain_ref[...]
    vec_out[0:1, :] = gain * (1.0 + mod_ref[0:1, model : 2 * model])
    vec_out[1:2, :] = mod_ref[0:1, 0:model]
    vec_out[2:3, :] = mod_ref[0:1, 2 * model : 3 * model]
    scale = gain * (1.0 + mod_ref[1:2, model : 2 * model])
    shift = mod_ref[1:2, 0:model]
    rows = ctx_ref[...].astype(F32)
    hid_ref[...] = (rows * rms_scale(rows) * scale + shift).astype(BF16)
    keys = jnp.dot(hid_ref[...], wk_ref[...], preferred_element_type=F32)
    kv_out[:, KV_HEADS * HEAD :] = jnp.dot(
        hid_ref[...], wv_ref[...], preferred_element_type=F32
    ).astype(BF16)
    for h in range(KV_HEADS):
        k = keys[:, h * HEAD : (h + 1) * HEAD]
        kv_out[:, h * HEAD : (h + 1) * HEAD] = (k * rms_scale(k) * kgain_ref[...]).astype(BF16)


def turn(v, table_ref, first, group, groups):
    turned = jnp.where(first, pltpu.roll(v, HEAD - 32, 1), pltpu.roll(v, 32, 1))
    parts = []
    for i in range(groups):
        rows = slice(i * GROUP_ROWS, (i + 1) * GROUP_ROWS)
        at = pl.ds((group + i) * GROUP_ROWS, GROUP_ROWS)
        parts.append((v[rows] * table_ref[0, at, :] + turned[rows] * table_ref[1, at, :]).astype(BF16))
    return jnp.concatenate(parts, axis=0)


def project_kernel(
    low_ref, mid_ref, high_ref, vec_ref, wk_ref, wv_ref, qgain_ref, kgain_ref,
    row_ref, col_ref, wq_ref,
    q_out, k_out, v_out, hid_ref, table_ref,
):
    own = mid_ref.shape[0]
    rows = own + 2 * WINDOW
    scale = vec_ref[0:1, :]
    shift = vec_ref[1:2, :]
    at = 0
    for ref in (low_ref, mid_ref, high_ref):
        for r in range(0, ref.shape[0], 32):
            v = ref[r : r + 32, :].astype(F32)
            hid_ref[at : at + 32, :] = (v * rms_scale(v) * scale + shift).astype(BF16)
            at += 32
    block = lax.axis_index(AXES) * (own // GROUP_ROWS) - WINDOW // GROUP_ROWS
    first_row = lax.shift_right_arithmetic(block, 1)
    for i in range(rows // GROUP_ROWS):
        row = lax.shift_right_arithmetic(block + i, 1) - first_row
        half = lax.bitwise_and(block + i, 1) * GROUP_ROWS
        for t in range(2):
            table_ref[t, i * GROUP_ROWS : (i + 1) * GROUP_ROWS, :] = (
                row_ref[t, pl.ds(row, 1), :] + col_ref[t, pl.ds(half, GROUP_ROWS), :]
            )
    lane = lax.broadcasted_iota(jnp.int32, (1, HEAD), 1)
    first = (lane % 64) < 32
    v_out[...] = jnp.dot(hid_ref[...], wv_ref[...], preferred_element_type=F32).astype(BF16)
    keys = jnp.dot(hid_ref[...], wk_ref[...], preferred_element_type=F32)
    kgain = kgain_ref[...]
    for h in range(KV_HEADS):
        k = keys[:, h * HEAD : (h + 1) * HEAD]
        k = k * rms_scale(k) * kgain
        k_out[:, h * HEAD : (h + 1) * HEAD] = turn(k, table_ref, first, 0, rows // GROUP_ROWS)
    qgain = qgain_ref[...]
    for pair in range(HEADS // 2):
        at = pair * 2 * HEAD
        both = jnp.dot(
            hid_ref[WINDOW : WINDOW + own, :], wq_ref[:, at : at + 2 * HEAD],
            preferred_element_type=F32,
        )
        for h in range(2):
            q = both[:, h * HEAD : (h + 1) * HEAD]
            q = q * rms_scale(q) * qgain
            q = turn(q, table_ref, first, WINDOW // GROUP_ROWS, own // GROUP_ROWS)
            for c in range(own // CHUNK):
                q_out[c, 2 * pair + h] = q[c * CHUNK : (c + 1) * CHUNK]


def attend_kernel(
    sink_ref, q_ref, k_ref, v_ref, x0_ref, x1_ref, x2_ref, x3_ref, lat_ref, vec_ref,
    wo_ref, out_hbm, mix_ref, vals_ref, ctx_ref, out_ref, out_sems,
):
    start = lax.axis_index(AXES) * lat_ref.shape[0]
    total_rows = lat_ref.shape[0] * lax.axis_size(AXES)
    chunks = q_ref.shape[0]
    rows = k_ref.shape[0]
    far = ctx_ref.shape[0]
    for i, ref in enumerate((x0_ref, x1_ref, x2_ref, x3_ref)):
        n = ref.shape[0]
        ctx_ref[i * n : (i + 1) * n, :] = ref[...]
    width = CHUNK + 2 * WINDOW
    factor = HEAD ** (-0.5) * LOG2E
    kv = KV_HEADS * HEAD
    for g in range(KV_HEADS):
        vals_ref[g, 0:rows, 0:HEAD] = v_ref[:, g * HEAD : (g + 1) * HEAD]
        vals_ref[g, rows : rows + far, 0:HEAD] = ctx_ref[:, kv + g * HEAD : kv + (g + 1) * HEAD]
        vals_ref[g, :, HEAD:] = jnp.ones_like(vals_ref[g, :, HEAD:])
    row = lax.broadcasted_iota(jnp.int32, (CHUNK, width), 0)
    col = lax.broadcasted_iota(jnp.int32, (CHUNK, width), 1)
    nt = (((1,), (1,)), ((), ()))
    for c in range(chunks):
        pos = start - WINDOW + c * CHUNK + col
        allowed = (col >= row) & (col <= row + 2 * WINDOW) & (pos >= 0) & (pos < total_rows)
        bias = jnp.where(allowed, 0.0, FAR_LOGIT)
        for g in range(KV_HEADS):
            q = q_ref[c, g * GROUP : (g + 1) * GROUP].reshape(GROUP * CHUNK, HEAD)
            k = k_ref[c * CHUNK : c * CHUNK + width, g * HEAD : (g + 1) * HEAD]
            near = lax.dot_general(q, k, nt, preferred_element_type=F32)
            near = near.reshape(GROUP, CHUNK, width) + bias[None]
            ctx = lax.dot_general(
                q, ctx_ref[:, g * HEAD : (g + 1) * HEAD], nt, preferred_element_type=F32
            ).reshape(GROUP, CHUNK, far)
            sink = jnp.concatenate(
                [
                    jnp.broadcast_to(sink_ref[:, g * GROUP + h : g * GROUP + h + 1], (CHUNK, 1))[None]
                    for h in range(GROUP)
                ],
                axis=0,
            ) * (HEAD**0.5)
            top = jnp.maximum(
                jnp.maximum(
                    jnp.max(near, axis=-1, keepdims=True), jnp.max(ctx, axis=-1, keepdims=True)
                ),
                sink,
            )
            near = jnp.exp2((near - top) * factor).astype(BF16).reshape(GROUP * CHUNK, width)
            ctx = jnp.exp2((ctx - top) * factor).astype(BF16).reshape(GROUP * CHUNK, far)
            tail = jnp.exp2((sink - top) * factor).reshape(GROUP * CHUNK, 1)
            mixed = jnp.dot(
                near, vals_ref[g, c * CHUNK : c * CHUNK + width, :], preferred_element_type=F32
            ) + jnp.dot(ctx, vals_ref[g, rows : rows + far, :], preferred_element_type=F32)
            mixed = (mixed[:, :HEAD] / (mixed[:, HEAD:] + tail)).astype(BF16)
            for h in range(GROUP):
                at = (g * GROUP + h) * HEAD
                mix_ref[c * CHUNK : (c + 1) * CHUNK, at : at + HEAD] = mixed[
                    h * CHUNK : (h + 1) * CHUNK
                ]
    model = out_ref.shape[1]
    step = 256
    copies = []
    for i, at in enumerate(range(0, model, step)):
        update = jnp.dot(mix_ref[...], wo_ref[:, at : at + step], preferred_element_type=F32)
        out_ref[:, at : at + step] = (
            lat_ref[:, at : at + step].astype(F32) + vec_ref[2:3, at : at + step] * update
        ).astype(BF16)
        columns = pl.ds(at, step)
        copy = pltpu.make_async_copy(
            out_ref.at[:, columns], out_hbm.at[:, columns], out_sems.at[i]
        )
        copy.start()
        copies.append(copy)
    for copy in copies:
        copy.wait()


def call(kernel, outs, scratch, limit, flops, *args, hbm=(), out_hbm=False):
    vmem = pl.BlockSpec(memory_space=pltpu.VMEM)
    many = isinstance(outs, (list, tuple))
    specs = [vmem] * len(args)
    out_spec = pl.BlockSpec(memory_space=pltpu.HBM) if out_hbm else vmem
    for i in hbm:
        specs[i] = pl.BlockSpec(memory_space=pltpu.HBM)
    return pl.pallas_call(
        kernel,
        out_shape=outs,
        in_specs=specs,
        out_specs=[vmem] * len(outs) if many else out_spec,
        scratch_shapes=scratch,
        compiler_params=pltpu.CompilerParams(vmem_limit_bytes=limit),
        cost_estimate=pl.CostEstimate(flops=flops, bytes_accessed=flops // 256, transcendentals=0),
    )(*args)


def rotary_tables(row_positions, col_positions):
    quarter = HEAD // 4
    inverse = jnp.power(ROPE_BASE, -jnp.arange(quarter, dtype=F32) / quarter)
    sign = jnp.where(jnp.arange(HEAD // 2) < HEAD // 4, -1.0, 1.0)

    def table(positions):
        angles = positions.astype(F32)[:, None] * inverse
        angles = jnp.concatenate([angles, angles], axis=-1)
        return jnp.stack([jnp.cos(angles), jnp.sin(angles) * sign])

    by_rows = table(row_positions)
    by_cols = table(col_positions)
    none = ((0, 0), (0, 0))
    return (
        jnp.pad(by_rows, (*none, (0, HEAD // 2))),
        jnp.pad(by_cols, (*none, (HEAD // 2, 0))),
    )


def spread(array, axis):
    size = lax.axis_size(axis)
    return [array] + [
        lax.ppermute(array, axis, [(i, (i + k) % size) for i in range(size)])
        for k in range(1, size)
    ]


def local(
    latent,
    context,
    condition,
    context_condition,
    modulation_weight,
    norm_gain,
    query_weight,
    key_weight,
    value_weight,
    output_weight,
    query_gain,
    key_gain,
    sink_logit,
):
    own, model = latent.shape
    width = modulation_weight.shape[1]
    kv = key_weight.shape[1]
    world = lax.axis_size(AXES)
    members = lax.axis_size(FIRST)
    start = lax.axis_index(AXES) * own
    up = [(i, i + 1) for i in range(world - 1)]
    down = [(i + 1, i) for i in range(world - 1)]
    struct = jax.ShapeDtypeStruct
    span = own + 2 * WINDOW

    payload = call(
        partial_kernel,
        struct((members, 8, width), BF16),
        [
            pltpu.VMEM((1, condition.shape[0]), F32),
            pltpu.VMEM((1, condition.shape[0]), F32),
            pltpu.VMEM(modulation_weight.shape, BF16),
            pltpu.VMEM((1, model), BF16),
            pltpu.VMEM((8, condition.shape[0]), F32),
            pltpu.VMEM((8, width), F32),
            pltpu.SemaphoreType.DMA((4,)),
        ],
        ALL_VMEM, 1000,
        condition[None], context_condition[None], modulation_weight, context,
        hbm=(0, 1, 2, 3),
    )
    first = exchange(payload, FIRST)
    low, high = call(
        edges_kernel,
        [struct((WINDOW, model), BF16), struct((WINDOW, model), BF16)],
        [pltpu.SemaphoreType.DMA((2,))],
        ALL_VMEM - 1300 * 1024, 1000,
        latent,
        hbm=(0,),
    )
    below = lax.ppermute(high, AXES, up)
    above = lax.ppermute(low, AXES, down)
    payload, ctx_rows = call(
        middle_kernel,
        [struct((lax.axis_size(SECOND), 8, width), BF16), struct((members, model), BF16)],
        [pltpu.VMEM((16, width), F32), pltpu.VMEM((members, model), F32)],
        4 * MIB, 1000,
        first,
    )
    second = exchange(payload, SECOND)
    ctx_parts = spread(ctx_rows, "x")
    ctx_rows = call(join_kernel, struct((4 * members, model), BF16), [], 2 * MIB, 1000, *ctx_parts)
    modulation = call(
        vectors_kernel,
        struct((8, 3 * model), F32),
        [pltpu.VMEM((8, width), F32)],
        4 * MIB, 4_000_000_000,
        second,
    )
    first_row = lax.div(start - WINDOW, GRID_W).astype(jnp.int32)
    modulation, row_positions, col_positions = lax.optimization_barrier(
        (
            modulation,
            first_row + jnp.arange(16, dtype=jnp.int32),
            jnp.arange(GRID_W, dtype=jnp.int32),
        )
    )
    by_rows, by_cols = rotary_tables(row_positions, col_positions)
    ctx_kv, vectors = call(
        context_kernel,
        [struct((4 * members, 2 * kv), BF16), struct((8, model), F32)],
        [pltpu.VMEM((4 * members, model), BF16)],
        8 * MIB, 4_000_000_000,
        modulation, ctx_rows, norm_gain[None], key_weight, value_weight, key_gain[None],
    )
    ctx_all = spread(ctx_kv, "y")
    queries, keys, values = call(
        project_kernel,
        [
            struct((own // CHUNK, HEADS, CHUNK, HEAD), BF16),
            struct((span, kv), BF16),
            struct((span, kv), BF16),
        ],
        [
            pltpu.VMEM((span, model), BF16),
            pltpu.VMEM((2, span, HEAD), F32),
        ],
        20 * MIB, 6_000_000_000,
        below, latent, above, vectors, key_weight, value_weight, query_gain[None], key_gain[None],
        by_rows, by_cols, query_weight,
    )
    return call(
        attend_kernel,
        struct((own, model), BF16),
        [
            pltpu.VMEM((own, HEADS * HEAD), BF16),
            pltpu.VMEM((KV_HEADS, span + world, 2 * HEAD), BF16),
            pltpu.VMEM((world, 2 * kv), BF16),
            pltpu.VMEM((own, model), BF16),
            pltpu.SemaphoreType.DMA((8,)),
        ],
        20 * MIB, 3_000_000_000,
        sink_logit[None], queries, keys, values, *ctx_all, latent, vectors, output_weight,
        out_hbm=True,
    )


def solution(mesh):
    torus = Mesh(mesh.devices.reshape(8, 4, 4, 2), AXES)
    rows = P(AXES, None)
    in_specs = (
        rows,
        rows,
        P(("z", "x")),
        P(("z", "x")),
        P(("z", "x"), ("y", "c")),
        P(),
        P(),
        P(),
        P(),
        P(),
        P(),
        P(),
        P(),
    )
    return jax.shard_map(local, mesh=torus, in_specs=in_specs, out_specs=rows, check_vma=False)
```

```python
import jax
import jax.numpy as jnp
from jax import lax
from jax.experimental import pallas as pl
from jax.experimental.pallas import tpu as pltpu
from jax.sharding import Mesh
from jax.sharding import PartitionSpec as P

WINDOW = 128
GRID_W = 64
HEAD = 128
HEADS = 8
KV_HEADS = 2
GROUP = HEADS // KV_HEADS
CHUNK = 96
EPS = 1e-06
ROPE_BASE = 10000.0
FAR_LOGIT = -1e30
LOG2E = 1.4426950408889634
MIB = 1024 * 1024
ALL_VMEM = 67_043_328
GROUP_ROWS = 32

AXES = ("z", "x", "y", "c")
FIRST = ("z", "c")
SECOND = ("x", "y")

F32 = jnp.float32
BF16 = jnp.bfloat16


def rms_scale(v):
    return lax.rsqrt(jnp.mean(v * v, axis=-1, keepdims=True) + EPS)


def high_low(v):
    high = v.astype(BF16).astype(F32)
    return high, v - high


def exchange(array, axes):
    return lax.all_to_all(array, axes, split_axis=0, concat_axis=0, tiled=True)


def copy_all(pairs, sems):
    copies = [
        pltpu.make_async_copy(src, dst, sems.at[i]) for i, (src, dst) in enumerate(pairs)
    ]
    for copy in copies:
        copy.start()
    return copies


def partial_kernel(
    cond_hbm, cctx_hbm, weight_hbm, ctx_hbm, out_ref,
    cond_ref, cctx_ref, weight_ref, ctx_ref, act_ref, rows_ref, sems,
):
    copies = copy_all(
        [(cond_hbm, cond_ref), (cctx_hbm, cctx_ref), (weight_hbm, weight_ref), (ctx_hbm, ctx_ref)],
        sems,
    )
    width = weight_ref.shape[1]
    model = ctx_ref.shape[1]
    act_ref[...] = jnp.zeros_like(act_ref)
    rows_ref[...] = jnp.zeros_like(rows_ref)
    for copy in copies:
        copy.wait()
    act_ref[0:1, :] = jax.nn.silu(cond_ref[...])
    act_ref[1:2, :] = jax.nn.silu(cctx_ref[...])
    part = jnp.dot(act_ref[...].astype(BF16), weight_ref[...], preferred_element_type=F32)
    high, low = high_low(part)
    rows_ref[0:2, :] = high[0:2]
    rows_ref[2:4, :] = low[0:2]
    ctx = ctx_ref[...].astype(F32)
    for i in range(3):
        size = min(width, model - i * width)
        rows_ref[4 + i : 5 + i, 0:size] = ctx[:, i * width : i * width + size]
    packed = rows_ref[...].astype(BF16)
    for i in range(out_ref.shape[0]):
        out_ref[i] = packed


def edges_kernel(lat_hbm, low_ref, high_ref, sems):
    own = lat_hbm.shape[0]
    copies = copy_all(
        [
            (lat_hbm.at[pl.ds(0, WINDOW)], low_ref),
            (lat_hbm.at[pl.ds(own - WINDOW, WINDOW)], high_ref),
        ],
        sems,
    )
    for copy in copies:
        copy.wait()


def middle_kernel(in_ref, out_ref, ctx_out, rows_ref, ctx_ref):
    members, _, width = in_ref.shape
    model = ctx_out.shape[1]
    for c in range(2):
        total = None
        for z in range(members // 2):
            m = 2 * z + c
            rows = in_ref[m].astype(F32)
            total = rows if total is None else total + rows
            for i in range(3):
                size = min(width, model - i * width)
                ctx_ref[m : m + 1, i * width : i * width + size] = rows[4 + i : 5 + i, 0:size]
        rows_ref[0:8, :] = total
        high, low = high_low(rows_ref[0:2, :] + rows_ref[2:4, :])
        rows_ref[8 + 4 * c : 10 + 4 * c, :] = high
        rows_ref[10 + 4 * c : 12 + 4 * c, :] = low
    packed = rows_ref[8:16, :].astype(BF16)
    for i in range(out_ref.shape[0]):
        out_ref[i] = packed
    ctx_out[...] = ctx_ref[...].astype(BF16)


def vectors_kernel(
    second_ref, low_hbm, mod_out, low_ref, tmp_ref, sems
):
    copies = copy_all([(low_hbm, low_ref)], sems)
    members, _, width = second_ref.shape
    side = 4
    for y in range(side):
        total = second_ref[y].astype(F32)
        for x in range(1, members // side):
            total += second_ref[x * side + y].astype(F32)
        tmp_ref[...] = total
        for c in range(2):
            at = (2 * y + c) * width
            mod_out[0:2, at : at + width] = (
                tmp_ref[4 * c : 4 * c + 2, :] + tmp_ref[4 * c + 2 : 4 * c + 4, :]
            )
    copies[0].wait()


def join_kernel(c0_ref, c1_ref, c2_ref, c3_ref, out_ref):
    for i, ref in enumerate((c0_ref, c1_ref, c2_ref, c3_ref)):
        n = ref.shape[0]
        out_ref[i * n : (i + 1) * n, :] = ref[...]


def context_kernel(
    mod_ref, ctx_ref, gain_ref, wk_ref, wv_ref, kgain_ref, kv_out, vec_out, hid_ref
):
    model = gain_ref.shape[1]
    gain = gain_ref[...]
    vec_out[0:1, :] = gain * (1.0 + mod_ref[0:1, model : 2 * model])
    vec_out[1:2, :] = mod_ref[0:1, 0:model]
    vec_out[2:3, :] = mod_ref[0:1, 2 * model : 3 * model]
    scale = gain * (1.0 + mod_ref[1:2, model : 2 * model])
    shift = mod_ref[1:2, 0:model]
    rows = ctx_ref[...].astype(F32)
    hid_ref[...] = (rows * rms_scale(rows) * scale + shift).astype(BF16)
    keys = jnp.dot(hid_ref[...], wk_ref[...], preferred_element_type=F32)
    kv_out[:, KV_HEADS * HEAD :] = jnp.dot(
        hid_ref[...], wv_ref[...], preferred_element_type=F32
    ).astype(BF16)
    for h in range(KV_HEADS):
        k = keys[:, h * HEAD : (h + 1) * HEAD]
        kv_out[:, h * HEAD : (h + 1) * HEAD] = (k * rms_scale(k) * kgain_ref[...]).astype(BF16)


def turn(v, table_ref, first, group, groups):
    turned = jnp.where(first, pltpu.roll(v, HEAD - 32, 1), pltpu.roll(v, 32, 1))
    parts = []
    for i in range(groups):
        rows = slice(i * GROUP_ROWS, (i + 1) * GROUP_ROWS)
        at = pl.ds((group + i) * GROUP_ROWS, GROUP_ROWS)
        parts.append((v[rows] * table_ref[0, at, :] + turned[rows] * table_ref[1, at, :]).astype(BF16))
    return jnp.concatenate(parts, axis=0)


def project_kernel(
    low_ref, mid_ref, high_ref, vec_ref, wk_ref, wv_ref, qgain_ref, kgain_ref,
    row_ref, col_ref, wq_ref,
    q_out, k_out, v_out, hid_ref, table_ref,
):
    own = mid_ref.shape[0]
    rows = own + 2 * WINDOW
    scale = vec_ref[0:1, :]
    shift = vec_ref[1:2, :]
    at = 0
    for ref in (low_ref, mid_ref, high_ref):
        for r in range(0, ref.shape[0], 32):
            v = ref[r : r + 32, :].astype(F32)
            hid_ref[at : at + 32, :] = (v * rms_scale(v) * scale + shift).astype(BF16)
            at += 32
    block = lax.axis_index(AXES) * (own // GROUP_ROWS) - WINDOW // GROUP_ROWS
    first_row = lax.shift_right_arithmetic(block, 1)
    for i in range(rows // GROUP_ROWS):
        row = lax.shift_right_arithmetic(block + i, 1) - first_row
        half = lax.bitwise_and(block + i, 1) * GROUP_ROWS
        for t in range(2):
            table_ref[t, i * GROUP_ROWS : (i + 1) * GROUP_ROWS, :] = (
                row_ref[t, pl.ds(row, 1), :] + col_ref[t, pl.ds(half, GROUP_ROWS), :]
            )
    lane = lax.broadcasted_iota(jnp.int32, (1, HEAD), 1)
    first = (lane % 64) < 32
    v_out[...] = jnp.dot(hid_ref[...], wv_ref[...], preferred_element_type=F32).astype(BF16)
    keys = jnp.dot(hid_ref[...], wk_ref[...], preferred_element_type=F32)
    kgain = kgain_ref[...]
    for h in range(KV_HEADS):
        k = keys[:, h * HEAD : (h + 1) * HEAD]
        k = k * rms_scale(k) * kgain
        k_out[:, h * HEAD : (h + 1) * HEAD] = turn(k, table_ref, first, 0, rows // GROUP_ROWS)
    qgain = qgain_ref[...]
    for pair in range(HEADS // 2):
        at = pair * 2 * HEAD
        both = jnp.dot(
            hid_ref[WINDOW : WINDOW + own, :], wq_ref[:, at : at + 2 * HEAD],
            preferred_element_type=F32,
        )
        for h in range(2):
            q = both[:, h * HEAD : (h + 1) * HEAD]
            q = q * rms_scale(q) * qgain
            q = turn(q, table_ref, first, WINDOW // GROUP_ROWS, own // GROUP_ROWS)
            for c in range(own // CHUNK):
                q_out[c, 2 * pair + h] = q[c * CHUNK : (c + 1) * CHUNK]


def attend_kernel(
    sink_ref, q_ref, k_ref, v_ref, x0_ref, x1_ref, x2_ref, x3_ref, lat_ref, vec_ref,
    wo_ref, out_hbm, mix_ref, vals_ref, ctx_ref, out_ref, out_sems,
):
    start = lax.axis_index(AXES) * lat_ref.shape[0]
    total_rows = lat_ref.shape[0] * lax.axis_size(AXES)
    chunks = q_ref.shape[0]
    rows = k_ref.shape[0]
    far = ctx_ref.shape[0]
    for i, ref in enumerate((x0_ref, x1_ref, x2_ref, x3_ref)):
        n = ref.shape[0]
        ctx_ref[i * n : (i + 1) * n, :] = ref[...]
    width = CHUNK + 2 * WINDOW
    factor = HEAD ** (-0.5) * LOG2E
    kv = KV_HEADS * HEAD
    for g in range(KV_HEADS):
        vals_ref[g, 0:rows, 0:HEAD] = v_ref[:, g * HEAD : (g + 1) * HEAD]
        vals_ref[g, rows : rows + far, 0:HEAD] = ctx_ref[:, kv + g * HEAD : kv + (g + 1) * HEAD]
        vals_ref[g, :, HEAD:] = jnp.ones_like(vals_ref[g, :, HEAD:])
    row = lax.broadcasted_iota(jnp.int32, (CHUNK, width), 0)
    col = lax.broadcasted_iota(jnp.int32, (CHUNK, width), 1)
    nt = (((1,), (1,)), ((), ()))
    for c in range(chunks):
        pos = start - WINDOW + c * CHUNK + col
        allowed = (col >= row) & (col <= row + 2 * WINDOW) & (pos >= 0) & (pos < total_rows)
        bias = jnp.where(allowed, 0.0, FAR_LOGIT)
        for g in range(KV_HEADS):
            q = q_ref[c, g * GROUP : (g + 1) * GROUP].reshape(GROUP * CHUNK, HEAD)
            k = k_ref[c * CHUNK : c * CHUNK + width, g * HEAD : (g + 1) * HEAD]
            near = lax.dot_general(q, k, nt, preferred_element_type=F32)
            near = near.reshape(GROUP, CHUNK, width) + bias[None]
            ctx = lax.dot_general(
                q, ctx_ref[:, g * HEAD : (g + 1) * HEAD], nt, preferred_element_type=F32
            ).reshape(GROUP, CHUNK, far)
            sink = jnp.concatenate(
                [
                    jnp.broadcast_to(sink_ref[:, g * GROUP + h : g * GROUP + h + 1], (CHUNK, 1))[None]
                    for h in range(GROUP)
                ],
                axis=0,
            ) * (HEAD**0.5)
            top = jnp.maximum(
                jnp.maximum(
                    jnp.max(near, axis=-1, keepdims=True), jnp.max(ctx, axis=-1, keepdims=True)
                ),
                sink,
            )
            near = jnp.exp2((near - top) * factor).astype(BF16).reshape(GROUP * CHUNK, width)
            ctx = jnp.exp2((ctx - top) * factor).astype(BF16).reshape(GROUP * CHUNK, far)
            tail = jnp.exp2((sink - top) * factor).reshape(GROUP * CHUNK, 1)
            mixed = jnp.dot(
                near, vals_ref[g, c * CHUNK : c * CHUNK + width, :], preferred_element_type=F32
            ) + jnp.dot(ctx, vals_ref[g, rows : rows + far, :], preferred_element_type=F32)
            mixed = (mixed[:, :HEAD] / (mixed[:, HEAD:] + tail)).astype(BF16)
            for h in range(GROUP):
                at = (g * GROUP + h) * HEAD
                mix_ref[c * CHUNK : (c + 1) * CHUNK, at : at + HEAD] = mixed[
                    h * CHUNK : (h + 1) * CHUNK
                ]
    model = out_ref.shape[1]
    step = 256
    copies = []
    for i, at in enumerate(range(0, model, step)):
        update = jnp.dot(mix_ref[...], wo_ref[:, at : at + step], preferred_element_type=F32)
        out_ref[:, at : at + step] = (
            lat_ref[:, at : at + step].astype(F32) + vec_ref[2:3, at : at + step] * update
        ).astype(BF16)
        columns = pl.ds(at, step)
        copy = pltpu.make_async_copy(
            out_ref.at[:, columns], out_hbm.at[:, columns], out_sems.at[i]
        )
        copy.start()
        copies.append(copy)
    for copy in copies:
        copy.wait()


def call(kernel, outs, scratch, limit, flops, *args, hbm=(), out_hbm=False):
    vmem = pl.BlockSpec(memory_space=pltpu.VMEM)
    many = isinstance(outs, (list, tuple))
    specs = [vmem] * len(args)
    out_spec = pl.BlockSpec(memory_space=pltpu.HBM) if out_hbm else vmem
    for i in hbm:
        specs[i] = pl.BlockSpec(memory_space=pltpu.HBM)
    return pl.pallas_call(
        kernel,
        out_shape=outs,
        in_specs=specs,
        out_specs=[vmem] * len(outs) if many else out_spec,
        scratch_shapes=scratch,
        compiler_params=pltpu.CompilerParams(vmem_limit_bytes=limit),
        cost_estimate=pl.CostEstimate(flops=flops, bytes_accessed=flops // 256, transcendentals=0),
    )(*args)


def rotary_tables(row_positions, col_positions):
    quarter = HEAD // 4
    inverse = jnp.power(ROPE_BASE, -jnp.arange(quarter, dtype=F32) / quarter)
    sign = jnp.where(jnp.arange(HEAD // 2) < HEAD // 4, -1.0, 1.0)

    def table(positions):
        angles = positions.astype(F32)[:, None] * inverse
        angles = jnp.concatenate([angles, angles], axis=-1)
        return jnp.stack([jnp.cos(angles), jnp.sin(angles) * sign])

    by_rows = table(row_positions)
    by_cols = table(col_positions)
    none = ((0, 0), (0, 0))
    return (
        jnp.pad(by_rows, (*none, (0, HEAD // 2))),
        jnp.pad(by_cols, (*none, (HEAD // 2, 0))),
    )


def spread(array, axis):
    size = lax.axis_size(axis)
    return [array] + [
        lax.ppermute(array, axis, [(i, (i + k) % size) for i in range(size)])
        for k in range(1, size)
    ]


def local(
    latent,
    context,
    condition,
    context_condition,
    modulation_weight,
    norm_gain,
    query_weight,
    key_weight,
    value_weight,
    output_weight,
    query_gain,
    key_gain,
    sink_logit,
):
    own, model = latent.shape
    width = modulation_weight.shape[1]
    kv = key_weight.shape[1]
    world = lax.axis_size(AXES)
    members = lax.axis_size(FIRST)
    start = lax.axis_index(AXES) * own
    up = [(i, i + 1) for i in range(world - 1)]
    down = [(i + 1, i) for i in range(world - 1)]
    struct = jax.ShapeDtypeStruct
    span = own + 2 * WINDOW

    payload = call(
        partial_kernel,
        struct((members, 8, width), BF16),
        [
            pltpu.VMEM((1, condition.shape[0]), F32),
            pltpu.VMEM((1, condition.shape[0]), F32),
            pltpu.VMEM(modulation_weight.shape, BF16),
            pltpu.VMEM((1, model), BF16),
            pltpu.VMEM((8, condition.shape[0]), F32),
            pltpu.VMEM((8, width), F32),
            pltpu.SemaphoreType.DMA((4,)),
        ],
        ALL_VMEM, 1000,
        condition[None], context_condition[None], modulation_weight, context,
        hbm=(0, 1, 2, 3),
    )
    first = exchange(payload, FIRST)
    low, high = call(
        edges_kernel,
        [struct((WINDOW, model), BF16), struct((WINDOW, model), BF16)],
        [pltpu.SemaphoreType.DMA((2,))],
        ALL_VMEM - 1300 * 1024, 1000,
        latent,
        hbm=(0,),
    )
    below = lax.ppermute(high, AXES, up)
    above = lax.ppermute(low, AXES, down)
    payload, ctx_rows = call(
        middle_kernel,
        [struct((lax.axis_size(SECOND), 8, width), BF16), struct((members, model), BF16)],
        [pltpu.VMEM((16, width), F32), pltpu.VMEM((members, model), F32)],
        4 * MIB, 1000,
        first,
    )
    second = exchange(payload, SECOND)
    ctx_parts = spread(ctx_rows, "x")
    ctx_rows = call(join_kernel, struct((4 * members, model), BF16), [], 2 * MIB, 1000, *ctx_parts)
    modulation, below = call(
        vectors_kernel,
        [struct((8, 3 * model), F32), struct((WINDOW, model), BF16)],
        [pltpu.VMEM((8, width), F32), pltpu.SemaphoreType.DMA((1,))],
        4 * MIB, 4_000_000_000,
        second, below,
        hbm=(1,),
    )
    first_row = lax.div(start - WINDOW, GRID_W).astype(jnp.int32)
    modulation, row_positions, col_positions = lax.optimization_barrier(
        (
            modulation,
            first_row + jnp.arange(16, dtype=jnp.int32),
            jnp.arange(GRID_W, dtype=jnp.int32),
        )
    )
    by_rows, by_cols = rotary_tables(row_positions, col_positions)
    ctx_kv, vectors = call(
        context_kernel,
        [struct((4 * members, 2 * kv), BF16), struct((8, model), F32)],
        [pltpu.VMEM((4 * members, model), BF16)],
        8 * MIB, 4_000_000_000,
        modulation, ctx_rows, norm_gain[None], key_weight, value_weight, key_gain[None],
    )
    ctx_all = spread(ctx_kv, "y")
    queries, keys, values = call(
        project_kernel,
        [
            struct((own // CHUNK, HEADS, CHUNK, HEAD), BF16),
            struct((span, kv), BF16),
            struct((span, kv), BF16),
        ],
        [
            pltpu.VMEM((span, model), BF16),
            pltpu.VMEM((2, span, HEAD), F32),
        ],
        20 * MIB, 6_000_000_000,
        below, latent, above, vectors, key_weight, value_weight, query_gain[None], key_gain[None],
        by_rows, by_cols, query_weight,
    )
    return call(
        attend_kernel,
        struct((own, model), BF16),
        [
            pltpu.VMEM((own, HEADS * HEAD), BF16),
            pltpu.VMEM((KV_HEADS, span + world, 2 * HEAD), BF16),
            pltpu.VMEM((world, 2 * kv), BF16),
            pltpu.VMEM((own, model), BF16),
            pltpu.SemaphoreType.DMA((8,)),
        ],
        20 * MIB, 3_000_000_000,
        sink_logit[None], queries, keys, values, *ctx_all, latent, vectors, output_weight,
        out_hbm=True,
    )


def solution(mesh):
    torus = Mesh(mesh.devices.reshape(8, 4, 4, 2), AXES)
    rows = P(AXES, None)
    in_specs = (
        rows,
        rows,
        P(("z", "x")),
        P(("z", "x")),
        P(("z", "x"), ("y", "c")),
        P(),
        P(),
        P(),
        P(),
        P(),
        P(),
        P(),
        P(),
    )
    return jax.shard_map(local, mesh=torus, in_specs=in_specs, out_specs=rows, check_vma=False)
```
